256 devices in a mesh: sp: 32 (over z, y), tp: 8 (over x, core).
Axes of the slice: x: 4, y: 4, z: 8, core: 2. Of those that a mesh axis runs over, the one named last changes fastest.
Arguments:
- stream: bfloat16 [8192, 2048], P('sp'), may hold values from -3 to 3
- first_group_queries: bfloat16 [8192, 512], P('sp', 'tp'), may hold values from -6 to 6
- first_group_keys: bfloat16 [8192, 512], P('sp', 'tp'), may hold values from -6 to 6
- first_group_values: bfloat16 [8192, 1024], P('sp', 'tp'), may hold values from -5.5 to 5.5
- first_gate_logits: bfloat16 [8192, 1024], P('sp', 'tp'), may hold values from -6 to 6
- first_decay_logits: bfloat16 [8192, 512], P('sp', 'tp'), may hold values from -4.75 to 14.5
- second_group_queries: bfloat16 [8192, 1024], P('sp', 'tp'), may hold values from -6 to 6
- second_group_keys: bfloat16 [8192, 1024], P('sp', 'tp'), may hold values from -6 to 6
- second_group_values: bfloat16 [8192, 1024], P('sp', 'tp'), may hold values from -5.5 to 5.5
- second_gate_logits: bfloat16 [8192, 1024], P('sp', 'tp'), may hold values from -6 to 6
- second_decay_logits: bfloat16 [8192, 1024], P('sp', 'tp'), may hold values from -4.75 to 14.5
- position_log_decay: float32 [8192], P('sp'), may hold values from -0.6932 to 0, as said below
- per_head_norm_gain: float32 [128], replicated, may hold values from 0.1 to 1.9
- first_output_weight: bfloat16 [1024, 2048], P('tp'), may hold values from -0.125 to 0.125
- second_output_weight: bfloat16 [1024, 2048], P('tp'), may hold values from -0.125 to 0.125
- feedforward_norm_gain: float32 [2048], replicated, may hold values from 0.1 to 1.9
- gate_weight: bfloat16 [2048, 5632], P('sp', 'tp'), may hold values from -0.125 to 0.125
- up_weight: bfloat16 [2048, 5632], P('sp', 'tp'), may hold values from -0.125 to 0.125
- down_weight: bfloat16 [5632, 2048], P('tp', 'sp'), may hold values from -0.078125 to 0.078125
Outputs:
- refined: bfloat16 [8192, 2048], P(('sp', 'tp'))
The draws below stay inside these ranges and needn't reach their ends.
Inputs may be any that keep to these rules, and one draw needn't show every extreme that they name: `position_log_decay`: most positions carry 0.
All inputs are finite; a program needn't handle non-finite values.
Results may differ from the reference program's by a relative error of at most 0.018.
Values may be sent and summed in bfloat16 or wider, within the bound.
No kernel may reach another device: no remote copies, remote signals or barrier semaphores. Data moves between devices by JAX's collectives and lax.ppermute only.
A program may use at most 64 MiB of HBM per device.

```python
import math
import jax
import jax.numpy as jnp
from jax import lax

D = 2048
FF = 5632
HA = 8
HB = 8
KEY_SIZE_FIRST = 64
KEY_SIZE_SECOND = 128
DV = 128
BLK = 64
TOK_DEV = 256
TOKENS = 8192
N_TP = 8


def decay_law(key, width, salt):
    seeds = jax.random.split(jax.random.fold_in(key, salt), 5)
    fast_share = 0.3
    chain_total = jnp.exp(jax.random.uniform(seeds[0], (width,), jnp.float32, math.log(0.5), math.log(8.0)))
    slow_offsets = jnp.log(TOKENS / (16.0 * chain_total)) + 0.5
    fast_offsets = jax.random.uniform(seeds[1], (width,), jnp.float32, 0.4, 1.75)
    fast_pick = jax.random.uniform(seeds[2], (width,), jnp.float32) < fast_share
    offsets = jnp.where(fast_pick, fast_offsets, slow_offsets)
    shifts = jax.random.uniform(seeds[3], (TOKENS // TOK_DEV, 1), jnp.float32, -1.0, 1.0)
    shifts = jnp.repeat(shifts, TOK_DEV, axis=0)
    noise = jnp.clip(jax.random.normal(seeds[4], (TOKENS, width), jnp.float32), -4.0, 4.0)
    return jnp.clip(offsets[None, :] + shifts + noise, -4.75, 14.5).astype(jnp.bfloat16)


def ramp_keys(key, width, salt):
    seeds = jax.random.split(jax.random.fold_in(key, salt), 3)
    noise = jnp.clip(jax.random.normal(seeds[0], (TOKENS, width), jnp.float32), -4.0, 4.0)
    sizes = jax.random.uniform(seeds[1], (width,), jnp.float32, 1.5, 2.0)
    signs = jnp.where(jax.random.randint(seeds[2], (width,), 0, 2) == 0, -1.0, 1.0).astype(jnp.float32)
    places = (jnp.arange(TOKENS, dtype=jnp.int32) % TOK_DEV).astype(jnp.float32)
    ramp = 2.0 * (places + 0.5) / TOK_DEV - 1.0
    return (noise + ramp[:, None] * (sizes * signs)[None, :]).astype(jnp.bfloat16)


def offset_values(key, width, salt):
    seeds = jax.random.split(jax.random.fold_in(key, salt), 3)
    noise = jnp.clip(jax.random.normal(seeds[0], (TOKENS, width), jnp.float32), -4.0, 4.0)
    sizes = jax.random.uniform(seeds[1], (width,), jnp.float32, 0.9, 1.3)
    signs = jnp.where(jax.random.randint(seeds[2], (width,), 0, 2) == 0, -1.0, 1.0).astype(jnp.float32)
    return (noise + (sizes * signs)[None, :]).astype(jnp.bfloat16)


def draw_first_decay_logits(key, part):
    return decay_law(key, HA * KEY_SIZE_FIRST, 17)


def draw_second_decay_logits(key, part):
    return decay_law(key, HB * KEY_SIZE_SECOND, 23)


def draw_first_group_keys(key, part):
    return ramp_keys(key, HA * KEY_SIZE_FIRST, 31)


def draw_second_group_keys(key, part):
    return ramp_keys(key, HB * KEY_SIZE_SECOND, 37)


def draw_first_group_values(key, part):
    return offset_values(key, HA * DV, 41)


def draw_second_group_values(key, part):
    return offset_values(key, HB * DV, 43)


def draw_position_log_decay(key, part):
    seeds = jax.random.split(jax.random.fold_in(key, 29), 3)
    chance = jax.random.randint(seeds[0], (TOKENS,), 0, max(TOKENS // 4, 2))
    forced = jax.random.randint(seeds[1], (), 0, TOKENS)
    places = jnp.arange(TOKENS, dtype=jnp.int32)
    struck = (chance == 0) | (places == forced)
    depth = jax.random.uniform(seeds[2], (TOKENS,), jnp.float32, math.log(0.5), math.log(0.8))
    return jnp.where(struck, depth, 0.0).astype(jnp.float32)


def steps_of(stream_key, dims, cuts, low, largest):
    loudness, own = 1.0, jax.random.fold_in(stream_key, 6)
    for dim, parts in cuts:
        heights = jnp.exp(jax.random.uniform(jax.random.fold_in(own, dim), (parts,), jnp.float32, low / len(cuts), largest / len(cuts)))
        loudness = loudness * jnp.repeat(heights, dims[dim] // parts).reshape([-1 if axis == dim else 1 for axis in range(len(dims))])
    return loudness


def normal_values(rng, extent, spread, most, shards=(), kind=jnp.bfloat16):
    values = jax.random.normal(rng, extent, jnp.float32) * spread
    if len(shards) > 0:
        values = steps_of(rng, extent, shards, -0.22, 0.18) * values
    return jnp.clip(values, min=-most, max=most).astype(kind)


def setup_inputs(seed: int = 0) -> dict:
    splits = jax.random.split(jax.random.key(seed), 20)
    return {
        "stream": normal_values(splits[0], (TOKENS, D), 0.5, 3.0, ((0, 32),)),
        "first_group_queries": normal_values(splits[1], (TOKENS, HA * KEY_SIZE_FIRST), 1.0, 6.0, ((0, 32), (1, 8))),
        "first_group_keys": draw_first_group_keys(jax.random.fold_in(splits[19], 71), 0),
        "first_group_values": draw_first_group_values(jax.random.fold_in(splits[19], 71), 0),
        "first_gate_logits": normal_values(splits[4], (TOKENS, HA * DV), 1.0, 6.0, ((0, 32), (1, 8))),
        "first_decay_logits": draw_first_decay_logits(jax.random.fold_in(splits[19], 71), 0),
        "second_group_queries": normal_values(splits[6], (TOKENS, HB * KEY_SIZE_SECOND), 1.0, 6.0, ((0, 32), (1, 8))),
        "second_group_keys": draw_second_group_keys(jax.random.fold_in(splits[19], 71), 0),
        "second_group_values": draw_second_group_values(jax.random.fold_in(splits[19], 71), 0),
        "second_gate_logits": normal_values(splits[9], (TOKENS, HB * DV), 1.0, 6.0, ((0, 32), (1, 8))),
        "second_decay_logits": draw_second_decay_logits(jax.random.fold_in(splits[19], 71), 0),
        "position_log_decay": draw_position_log_decay(jax.random.fold_in(splits[19], 71), 0),
        "per_head_norm_gain": jnp.clip(1.0 + 0.18 * jax.random.normal(splits[12], (DV,), jnp.float32), 0.1, 1.9),
        "first_output_weight": normal_values(splits[13], (HA * DV, D), ((HA + HB) * DV) ** -0.5, 0.125, ((0, 8),)),
        "second_output_weight": normal_values(splits[14], (HB * DV, D), ((HA + HB) * DV) ** -0.5, 0.125, ((0, 8),)),
        "feedforward_norm_gain": jnp.clip(1.0 + 0.18 * jax.random.normal(splits[15], (D,), jnp.float32), 0.1, 1.9),
        "gate_weight": normal_values(splits[16], (D, FF), D ** -0.5, 0.125, ((0, 32), (1, 8))),
        "up_weight": normal_values(splits[17], (D, FF), D ** -0.5, 0.125, ((0, 32), (1, 8))),
        "down_weight": normal_values(splits[18], (FF, D), FF ** -0.5, 0.078125, ((0, 8), (1, 32))),
    }


decay_softness = 16.0
norm_eps = 1e-06
highest = lax.Precision.HIGHEST

def channel_log_decays(decay_logits, position_log_decay, key_channels):
    channel_log_decay = jax.nn.log_sigmoid(decay_logits.astype(jnp.float32)) / decay_softness + position_log_decay[:, None]
    return channel_log_decay.reshape(decay_logits.shape[0], -1, key_channels)

def one_way(query_matrix, key_matrix, value_matrix, channel_log_decay, start_state):
    length, heads, key_channels = query_matrix.shape
    value_width = value_matrix.shape[-1]
    block_count = length // BLK

    def blocks(member):
        return member.reshape(block_count, BLK, heads, member.shape[-1]).transpose(0, 2, 1, 3)
    query_blocks = blocks(query_matrix)
    key_blocks = blocks(key_matrix)
    value_blocks = blocks(value_matrix)
    running = jnp.cumsum(blocks(channel_log_decay), axis=2)
    block_last = running[:, :, -1:, :]
    query_in = query_blocks * jnp.exp(running)
    key_in = key_blocks * jnp.exp(-running)
    key_end = key_blocks * jnp.exp(block_last - running)
    places = jnp.arange(BLK, dtype=jnp.int32)
    lower = places[:, None] >= places[None, :]
    scores = jnp.where(lower, jnp.einsum('nhid,nhjd->nhij', query_in, key_in, precision=highest), 0.0)
    local_out = jnp.einsum('nhij,nhjv->nhiv', scores, value_blocks, precision=highest)

    def advance(states, inputs):
        query_part, key_part, value_part, last_part = inputs
        emitted = jnp.einsum('hid,hdv->hiv', query_part, states, precision=highest)
        states = states * jnp.exp(last_part)[:, 0, :, None] + jnp.einsum('hjd,hjv->hdv', key_part, value_part, precision=highest)
        return (states, emitted)
    _, carried = lax.scan(advance, start_state, (query_in, key_end, value_blocks, block_last))
    return (local_out + carried).transpose(0, 2, 1, 3).reshape(length, heads, value_width)

def attend_group(query_matrix, key_matrix, value_matrix, gate_values, decay_logits, position_log_decay, per_head_norm_gain, key_channels):
    length = query_matrix.shape[0]
    channel_log_decay = channel_log_decays(decay_logits, position_log_decay, key_channels)
    query_f = query_matrix.astype(jnp.float32).reshape(length, -1, key_channels)
    key_f = key_matrix.astype(jnp.float32).reshape(length, -1, key_channels)
    value_f = value_matrix.astype(jnp.float32).reshape(length, -1, DV)
    heads = query_f.shape[1]
    zero_state = jnp.zeros((heads, key_channels, DV), jnp.float32)
    forward = one_way(query_f, key_f, value_f, channel_log_decay, zero_state)
    backward = jnp.flip(one_way(jnp.flip(query_f, 0), jnp.flip(key_f, 0), jnp.flip(value_f, 0), jnp.flip(channel_log_decay, 0), zero_state), 0)
    both = forward + backward
    scale = lax.rsqrt(lax.optimization_barrier(jnp.mean(both * both, axis=-1, keepdims=True)) + norm_eps)
    gated = both * scale * per_head_norm_gain * jax.nn.silu(gate_values.astype(jnp.float32).reshape(both.shape))
    return gated.reshape(length, heads * DV).astype(jnp.bfloat16)

def shard_sums(left_pairs, length, width):

    def add_shard(totals, shard):
        part = jnp.zeros((length, width), jnp.float32)
        for left, right in left_pairs:
            span = right.shape[0] // N_TP
            part = part + jnp.dot(lax.dynamic_slice_in_dim(left, shard * span, span, 1), lax.dynamic_slice_in_dim(right, shard * span, span, 0), preferred_element_type=jnp.float32)
        rounded = lax.optimization_barrier(part.astype(jnp.bfloat16))
        return (totals + rounded.astype(jnp.float32), None)
    totals, _ = lax.scan(add_shard, jnp.zeros((length, width), jnp.float32), jnp.arange(N_TP, dtype=jnp.int32))
    return totals

def reference(stream, first_group_queries, first_group_keys, first_group_values, first_gate_logits, first_decay_logits, second_group_queries, second_group_keys, second_group_values, second_gate_logits, second_decay_logits, position_log_decay, per_head_norm_gain, first_output_weight, second_output_weight, feedforward_norm_gain, gate_weight, up_weight, down_weight):
    length = stream.shape[0]
    first_group_output = attend_group(first_group_queries, first_group_keys, first_group_values, first_gate_logits, first_decay_logits, position_log_decay, per_head_norm_gain, KEY_SIZE_FIRST)
    second_group_output = attend_group(second_group_queries, second_group_keys, second_group_values, second_gate_logits, second_decay_logits, position_log_decay, per_head_norm_gain, KEY_SIZE_SECOND)
    residual = stream.astype(jnp.float32) + shard_sums(((first_group_output, first_output_weight), (second_group_output, second_output_weight)), length, D)
    scale = lax.rsqrt(lax.optimization_barrier(jnp.mean(residual * residual, axis=-1, keepdims=True)) + norm_eps)
    normed = (residual * scale * feedforward_norm_gain).astype(jnp.bfloat16)
    gate_sum = jnp.dot(normed, gate_weight, preferred_element_type=jnp.float32)
    up_sum = jnp.dot(normed, up_weight, preferred_element_type=jnp.float32)
    hidden = (jax.nn.silu(gate_sum) * up_sum).astype(jnp.bfloat16)
    down_sum = shard_sums(((hidden, down_weight),), length, D)
    return (residual + 0.5 * down_sum).astype(jnp.bfloat16)
```

```python
import jax
import jax.numpy as jnp
from jax import lax
from jax.experimental import pallas as pl
from jax.experimental.pallas import tpu as pltpu
from jax.sharding import Mesh
from jax.sharding import PartitionSpec as P

DV = 128
SP = ("z", "y")
TP = ("x", "c")
SIZES = {"z": 8, "y": 4, "x": 4, "c": 2}
HIGH = lax.Precision.HIGHEST
F32 = jnp.float32
BF16 = jnp.bfloat16

decay_softness = 16.0
norm_eps = 1e-06


def shift(value, axis, by):
    n = SIZES[axis]
    return lax.ppermute(value, axis, [(i, (i + by) % n) for i in range(n)])


def log_decays(decay_ref):
    d = decay_ref[...].astype(F32)
    return (jnp.minimum(d, 0.0) - jnp.log1p(jnp.exp(-jnp.abs(d)))) / decay_softness


def lower_mask(n):
    return lax.broadcasted_iota(jnp.int32, (n, n), 0) >= lax.broadcasted_iota(jnp.int32, (n, n), 1)


def position_sums(pos_ref):
    n = pos_ref.shape[1]
    rows = jnp.broadcast_to(pos_ref[...], (n, n))
    low = lower_mask(n)
    diag = lax.broadcasted_iota(jnp.int32, (n, n), 0) == lax.broadcasted_iota(jnp.int32, (n, n), 1)
    upto = jnp.sum(jnp.where(low, rows, 0.0), axis=1, keepdims=True)
    before = jnp.sum(jnp.where(low & ~diag, rows, 0.0), axis=1, keepdims=True)
    return upto, before


def running_sums(logd, upto, before):
    n = logd.shape[0]
    tri = jnp.where(lower_mask(n), 1.0, 0.0).astype(F32)
    cum = jnp.dot(tri, logd, precision=HIGH, preferred_element_type=F32)
    return cum + upto, (cum - logd) + before


def rows_contracted(a, b, precision=None):
    return lax.dot_general(
        a, b, (((0,), (0,)), ((), ())), precision=precision, preferred_element_type=F32
    )


def lanes_contracted(a, b):
    return lax.dot_general(a, b, (((1,), (1,)), ((), ())), preferred_element_type=F32)


def states_kernel(ka, va, da, kb, vb, db, pos, msg):
    upto, before = position_sums(pos)
    n = pos.shape[1]
    pos_total = jnp.sum(pos[...], axis=1, keepdims=True)
    ones = jnp.ones((n, DV), F32)
    at = 0
    for k_ref, v_ref, d_ref in ((kb, vb, db), (ka, va, da)):
        logd = log_decays(d_ref)
        upto_l, before_l = running_sums(logd, upto, before)
        total = upto_l[n - 1 : n, :]
        key = k_ref[...].astype(F32)
        value = v_ref[...]
        ahead = rows_contracted((key * jnp.exp(total - upto_l)).astype(BF16), value)
        behind = rows_contracted((key * jnp.exp(before_l)).astype(BF16), value)
        totals = rows_contracted(logd, ones, HIGH) + pos_total
        high = totals.astype(BF16).astype(F32)
        lane = lax.broadcasted_iota(jnp.int32, totals.shape, 1)
        both = jnp.where(lane < 64, high, totals - high)
        groups = logd.shape[1] // 8
        part = jnp.concatenate(
            [x.reshape(groups, 8, DV) for x in (ahead, behind, both)], axis=1
        )
        msg[at : at + groups] = part.astype(BF16)
        at += groups
    msg[at:] = jnp.zeros((msg.shape[0] - at, *msg.shape[1:]), BF16)


def scan_kernel(msg, out):
    n = msg.shape[0]
    blocks = msg[...].astype(F32)
    decay = jnp.exp(blocks[:, 16:24, 0:1] + blocks[:, 16:24, 64:65])
    run = jnp.zeros((8, DV), F32)
    ahead = []
    for k in range(n):
        ahead.append(run)
        run = run * decay[k] + blocks[k, 0:8, :]
    run = jnp.zeros((8, DV), F32)
    behind = []
    for k in reversed(range(n)):
        behind.append(run)
        run = run * decay[k] + blocks[k, 8:16, :]
    behind.reverse()
    for k in range(n):
        out[k] = jnp.concatenate([ahead[k], behind[k]], axis=0).astype(BF16)


def local_kernel(qa, ka, va, da, qb, kb, vb, db, pos, out, qf_out, qb_out):
    n = pos.shape[1]
    half = n // 2
    upto, before = position_sums(pos)
    low = lower_mask(half)
    up = lax.broadcasted_iota(jnp.int32, (half, half), 0) <= lax.broadcasted_iota(
        jnp.int32, (half, half), 1
    )
    for g, (q_ref, k_ref, v_ref, d_ref) in enumerate(((qa, ka, va, da), (qb, kb, vb, db))):
        inc, exc = running_sums(log_decays(d_ref), upto, before)
        q = q_ref[...].astype(F32)
        k = k_ref[...].astype(F32)
        total = inc[n - 1 : n, :]
        lo = 0 if g == 1 else 128
        width = q.shape[1]
        qf_out[:, lo : lo + width] = (q * jnp.exp(inc)).astype(BF16)
        qb_out[:, lo : lo + width] = (q * jnp.exp(total - exc)).astype(BF16)
        diag = []
        for b in range(2):
            s = slice(b * half, (b + 1) * half)
            m = inc[b * half + half // 2 - 1 : b * half + half // 2, :]
            ahead = lanes_contracted(
                (q[s] * jnp.exp(inc[s] - m)).astype(BF16), (k[s] * jnp.exp(m - inc[s])).astype(BF16)
            )
            behind = lanes_contracted(
                (q[s] * jnp.exp(m - exc[s])).astype(BF16), (k[s] * jnp.exp(exc[s] - m)).astype(BF16)
            )
            diag.append(jnp.where(low, ahead, 0.0) + jnp.where(up, behind, 0.0))
        m = inc[half - 1 : half, :]
        first, second = slice(0, half), slice(half, n)
        down = lanes_contracted(
            (q[second] * jnp.exp(inc[second] - m)).astype(BF16),
            (k[first] * jnp.exp(m - inc[first])).astype(BF16),
        )
        upper = lanes_contracted(
            (q[first] * jnp.exp(m - exc[first])).astype(BF16),
            (k[second] * jnp.exp(exc[second] - m)).astype(BF16),
        )
        weights = jnp.concatenate(
            [
                jnp.concatenate([diag[0], upper], axis=1),
                jnp.concatenate([down, diag[1]], axis=1),
            ],
            axis=0,
        ).astype(BF16)
        out[:, g * DV : (g + 1) * DV] = jnp.dot(weights, v_ref[...], preferred_element_type=F32)


def finish_kernel(local, qf, qb, states, ga, gb, gain, out):
    groups = states[...].astype(F32)[:24]
    ahead = groups[:, 0:8, :].reshape(192, DV).astype(BF16)
    behind = groups[:, 8:16, :].reshape(192, DV).astype(BF16)
    for g, gate_ref in enumerate((ga, gb)):
        lo, hi = (0, 128) if g == 1 else (128, 192)
        both = (
            local[:, g * DV : (g + 1) * DV]
            + jnp.dot(qf[:, lo:hi], ahead[lo:hi], preferred_element_type=F32)
            + jnp.dot(qb[:, lo:hi], behind[lo:hi], preferred_element_type=F32)
        )
        scale = lax.rsqrt(jnp.mean(both * both, axis=-1, keepdims=True) + norm_eps)
        gate = gate_ref[...].astype(F32)
        silu = gate / (1.0 + jnp.exp(-gate))
        out[:, g * DV : (g + 1) * DV] = (both * scale * gain[...] * silu).astype(BF16)


def call(kernel, out_shape, flops, *args):
    return pl.pallas_call(
        kernel,
        out_shape=out_shape,
        cost_estimate=pl.CostEstimate(flops=flops, bytes_accessed=10**6, transcendentals=10**5),
    )(*args)


def around_x(value):
    rows = value.shape[0] // 2
    left, right = shift(value, "x", 1), shift(value, "x", -1)
    far_top = shift(left[:rows], "x", 1)
    far_low = shift(right[rows:], "x", -1)
    return jnp.concatenate([value, left, right, far_top, far_low], axis=0)


def per_device(
    stream,
    first_group_queries,
    first_group_keys,
    first_group_values,
    first_gate_logits,
    first_decay_logits,
    second_group_queries,
    second_group_keys,
    second_group_values,
    second_gate_logits,
    second_decay_logits,
    position_log_decay,
    per_head_norm_gain,
    first_output_weight,
    second_output_weight,
    feedforward_norm_gain,
    gate_weight,
    up_weight,
    down_weight,
):
    tokens, width = stream.shape
    chips = SIZES["x"]
    part = tokens // (chips * 2)
    core = lax.axis_index("c")
    place = lax.axis_index("x")

    gate_up = lax.all_gather(
        jnp.concatenate([gate_weight, up_weight], axis=1), SP, axis=0, tiled=True
    )
    down_whole = lax.all_gather(down_weight, SP, axis=1, tiled=True)

    pos = position_log_decay.reshape(1, tokens)
    messages = call(
        states_kernel,
        jax.ShapeDtypeStruct((32, 24, DV), BF16),
        10**8,
        first_group_keys,
        first_group_values,
        first_decay_logits,
        second_group_keys,
        second_group_values,
        second_decay_logits,
        pos,
    )
    arrived = lax.all_to_all(messages, SP, 0, 0, tiled=True)

    out_own = jnp.concatenate([first_output_weight, second_output_weight], axis=0)
    out_same = around_x(out_own)
    out_other = shift(out_same, "c", 1)

    local, query_ahead, query_behind = call(
        local_kernel,
        (
            jax.ShapeDtypeStruct((tokens, 2 * DV), F32),
            jax.ShapeDtypeStruct((tokens, 192), BF16),
            jax.ShapeDtypeStruct((tokens, 192), BF16),
        ),
        2 * 10**8,
        first_group_queries,
        first_group_keys,
        first_group_values,
        first_decay_logits,
        second_group_queries,
        second_group_keys,
        second_group_values,
        second_decay_logits,
        pos,
    )
    scanned = call(scan_kernel, jax.ShapeDtypeStruct((32, 16, DV), BF16), 10**7, arrived)
    states = lax.all_to_all(scanned, SP, 0, 0, tiled=True)
    mixed = call(
        finish_kernel,
        jax.ShapeDtypeStruct((tokens, 2 * DV), BF16),
        10**8,
        local,
        query_ahead,
        query_behind,
        states,
        first_gate_logits,
        second_gate_logits,
        per_head_norm_gain.reshape(1, DV),
    )
    left, right, far = shift(mixed, "x", 1), shift(mixed, "x", -1), shift(mixed, "x", 2)
    mixed_same = jnp.concatenate([mixed, left, right, far], axis=1)
    mixed_other = shift(mixed_same, "c", 1)
    residual = (
        stream.astype(F32)
        + jnp.dot(mixed_same, out_same, preferred_element_type=F32)
        + jnp.dot(mixed_other, out_other, preferred_element_type=F32)
    )
    scale = lax.rsqrt(jnp.mean(residual * residual, axis=-1, keepdims=True) + norm_eps)
    normed = (residual * scale * feedforward_norm_gain).astype(BF16)
    sums = jnp.dot(normed, gate_up, preferred_element_type=F32)
    units = gate_weight.shape[1]
    hidden = (jax.nn.silu(sums[:, :units]) * sums[:, units:]).astype(BF16)

    by_core = hidden.reshape(chips, 2, part, units)

    def partial_sums(which):
        rows = lax.dynamic_index_in_dim(by_core, which, 1, keepdims=False).reshape(-1, units)
        return jnp.dot(rows, down_whole, preferred_element_type=F32).astype(BF16)

    theirs = shift(partial_sums(1 - core), "c", 1)
    pair = (partial_sums(core).astype(F32) + theirs.astype(F32)).astype(BF16)
    blocks = lax.all_to_all(pair.reshape(chips, part, width), "x", 0, 0, tiled=True)
    down_sum = jnp.sum(blocks.astype(F32), axis=0)
    own = lax.dynamic_slice_in_dim(residual, (place * 2 + core) * part, part, 0)
    return (own + 0.5 * down_sum).astype(BF16)


def solution(mesh):
    split = Mesh(mesh.devices.reshape(8, 4, 4, 2), ("z", "y", "x", "c"))
    placed = (
        P(SP, None),
        *(P(SP, TP),) * 10,
        P(SP),
        P(),
        P(TP, None),
        P(TP, None),
        P(),
        P(SP, TP),
        P(SP, TP),
        P(TP, SP),
    )
    return jax.shard_map(
        per_device, mesh=split, in_specs=placed, out_specs=P(SP + TP, None), check_vma=False
    )
```

```python
import functools

import jax
import jax.numpy as jnp
from jax import lax
from jax.experimental import pallas as pl
from jax.experimental.pallas import tpu as pltpu
from jax.sharding import Mesh
from jax.sharding import PartitionSpec as P

DV = 128
SP = ("z", "y")
TP = ("x", "c")
SIZES = {"z": 8, "y": 4, "x": 4, "c": 2}
HIGH = lax.Precision.HIGHEST
F32 = jnp.float32
BF16 = jnp.bfloat16


decay_softness = 16.0
norm_eps = 1e-06


def shift(value, axis, by):
    n = SIZES[axis]
    return lax.ppermute(value, axis, [(i, (i + by) % n) for i in range(n)])


def by_position(ref, n):
    value = ref[...].astype(F32)
    return value if value.shape[0] == n else value.T


def log_decays(decay_ref, n):
    d = by_position(decay_ref, n)
    return (jnp.minimum(d, 0.0) - jnp.log1p(jnp.exp(-jnp.abs(d)))) / decay_softness


def lower_mask(n):
    return lax.broadcasted_iota(jnp.int32, (n, n), 0) >= lax.broadcasted_iota(jnp.int32, (n, n), 1)


def position_sums(pos_ref):
    n = pos_ref.shape[1]
    rows = jnp.broadcast_to(pos_ref[...], (n, n))
    low = lower_mask(n)
    diag = lax.broadcasted_iota(jnp.int32, (n, n), 0) == lax.broadcasted_iota(jnp.int32, (n, n), 1)
    upto = jnp.sum(jnp.where(low, rows, 0.0), axis=1, keepdims=True)
    before = jnp.sum(jnp.where(low & ~diag, rows, 0.0), axis=1, keepdims=True)
    return upto, before


def running_sums(logd, upto, before):
    n = logd.shape[0]
    tri = jnp.where(lower_mask(n), 1.0, 0.0).astype(F32)
    cum = jnp.dot(tri, logd, precision=HIGH, preferred_element_type=F32)
    return cum + upto, (cum - logd) + before


def rows_contracted(a, b, precision=None):
    return lax.dot_general(
        a, b, (((0,), (0,)), ((), ())), precision=precision, preferred_element_type=F32
    )


def lanes_contracted(a, b):
    return lax.dot_general(a, b, (((1,), (1,)), ((), ())), preferred_element_type=F32)


def states_kernel(ka, va, da, kb, vb, db, pos, msg):
    upto, before = position_sums(pos)
    n = pos.shape[1]
    pos_total = jnp.sum(pos[...], axis=1, keepdims=True)
    ones = jnp.ones((n, DV), F32)
    at = 0
    for k_ref, v_ref, d_ref in ((kb, vb, db), (ka, va, da)):
        logd = log_decays(d_ref, n)
        upto_l, before_l = running_sums(logd, upto, before)
        total = upto_l[n - 1 : n, :]
        key = by_position(k_ref, n)
        value = v_ref[...]
        ahead = rows_contracted((key * jnp.exp(total - upto_l)).astype(BF16), value)
        behind = rows_contracted((key * jnp.exp(before_l)).astype(BF16), value)
        totals = rows_contracted(logd, ones, HIGH) + pos_total
        high = totals.astype(BF16).astype(F32)
        lane = lax.broadcasted_iota(jnp.int32, totals.shape, 1)
        both = jnp.where(lane < 64, high, totals - high)
        groups = logd.shape[1] // 8
        part = jnp.concatenate(
            [x.reshape(groups, 8, DV) for x in (ahead, behind, both)], axis=1
        )
        msg[at : at + groups] = part.astype(BF16)
        at += groups
    msg[at:] = jnp.zeros((msg.shape[0] - at, *msg.shape[1:]), BF16)


def scan_kernel(msg, out):
    n = msg.shape[0]
    blocks = msg[...].astype(F32)
    decay = jnp.exp(blocks[:, 16:24, 0:1] + blocks[:, 16:24, 64:65])
    run = jnp.zeros((8, DV), F32)
    ahead = []
    for k in range(n):
        ahead.append(run)
        run = run * decay[k] + blocks[k, 0:8, :]
    run = jnp.zeros((8, DV), F32)
    behind = []
    for k in reversed(range(n)):
        behind.append(run)
        run = run * decay[k] + blocks[k, 8:16, :]
    behind.reverse()
    for k in range(n):
        out[k] = jnp.concatenate([ahead[k], behind[k]], axis=0).astype(BF16)


def local_kernel(qa, ka, va, da, qb, kb, vb, db, pos, out, qf_out, qb_out):
    n = pos.shape[1]
    half = n // 2
    upto, before = position_sums(pos)
    low = lower_mask(half)
    up = lax.broadcasted_iota(jnp.int32, (half, half), 0) <= lax.broadcasted_iota(
        jnp.int32, (half, half), 1
    )
    for g, (q_ref, k_ref, v_ref, d_ref) in enumerate(((qa, ka, va, da), (qb, kb, vb, db))):
        inc, exc = running_sums(log_decays(d_ref, n), upto, before)
        q = by_position(q_ref, n)
        k = by_position(k_ref, n)
        total = inc[n - 1 : n, :]
        lo = 0 if g == 1 else 128
        width = q.shape[1]
        qf_out[:, lo : lo + width] = (q * jnp.exp(inc)).astype(BF16)
        qb_out[:, lo : lo + width] = (q * jnp.exp(total - exc)).astype(BF16)
        diag = []
        for b in range(2):
            s = slice(b * half, (b + 1) * half)
            m = inc[b * half + half // 2 - 1 : b * half + half // 2, :]
            ahead = lanes_contracted(
                (q[s] * jnp.exp(inc[s] - m)).astype(BF16), (k[s] * jnp.exp(m - inc[s])).astype(BF16)
            )
            behind = lanes_contracted(
                (q[s] * jnp.exp(m - exc[s])).astype(BF16), (k[s] * jnp.exp(exc[s] - m)).astype(BF16)
            )
            diag.append(jnp.where(low, ahead, 0.0) + jnp.where(up, behind, 0.0))
        m = inc[half - 1 : half, :]
        first, second = slice(0, half), slice(half, n)
        down = lanes_contracted(
            (q[second] * jnp.exp(inc[second] - m)).astype(BF16),
            (k[first] * jnp.exp(m - inc[first])).astype(BF16),
        )
        upper = lanes_contracted(
            (q[first] * jnp.exp(m - exc[first])).astype(BF16),
            (k[second] * jnp.exp(exc[second] - m)).astype(BF16),
        )
        weights = jnp.concatenate(
            [
                jnp.concatenate([diag[0], upper], axis=1),
                jnp.concatenate([down, diag[1]], axis=1),
            ],
            axis=0,
        ).astype(BF16)
        out[:, g * DV : (g + 1) * DV] = jnp.dot(weights, v_ref[...], preferred_element_type=F32)


def finish_kernel(local, qf, qb, states, ga, gb, gain, out):
    groups = states[...].astype(F32)[:24]
    ahead = groups[:, 0:8, :].reshape(192, DV).astype(BF16)
    behind = groups[:, 8:16, :].reshape(192, DV).astype(BF16)
    for g, gate_ref in enumerate((ga, gb)):
        lo, hi = (0, 128) if g == 1 else (128, 192)
        both = (
            local[:, g * DV : (g + 1) * DV]
            + jnp.dot(qf[:, lo:hi], ahead[lo:hi], preferred_element_type=F32)
            + jnp.dot(qb[:, lo:hi], behind[lo:hi], preferred_element_type=F32)
        )
        scale = lax.rsqrt(jnp.mean(both * both, axis=-1, keepdims=True) + norm_eps)
        gate = gate_ref[...].astype(F32)
        silu = gate / (1.0 + jnp.exp(-gate))
        out[:, g * DV : (g + 1) * DV] = (both * scale * gain[...] * silu).astype(BF16)


def call(kernel, out_shape, flops, *args):
    return pl.pallas_call(
        kernel,
        out_shape=out_shape,
        cost_estimate=pl.CostEstimate(flops=flops, bytes_accessed=10**6, transcendentals=10**5),
    )(*args)


ANY = pl.BlockSpec(memory_space=pl.ANY)
VMEM = pl.BlockSpec(memory_space=pltpu.VMEM)
SMEM = pl.BlockSpec(memory_space=pltpu.SMEM)
STRIP = 512


def residual_kernel(where, same, other, stream, gain, *refs):
    weights, (normed, own, scratch, rows, sems) = refs[:8], refs[8:]
    strips = stream.shape[1] // STRIP

    def copy(k, s):
        cols = slice(s * STRIP, (s + 1) * STRIP)
        return pltpu.make_async_copy(
            weights[k].at[:, cols], scratch.at[s, k * 256 : (k + 1) * 256, :], sems.at[s, k]
        )

    for s in range(strips):
        for k in range(8):
            copy(k, s).start()
    squares = jnp.zeros((stream.shape[0], 1), F32)
    for s in range(strips):
        for k in range(8):
            copy(k, s).wait()
        cols = slice(s * STRIP, (s + 1) * STRIP)
        part = (
            stream[:, cols].astype(F32)
            + jnp.dot(same[...], scratch[s, :1024, :], preferred_element_type=F32)
            + jnp.dot(other[...], scratch[s, 1024:, :], preferred_element_type=F32)
        )
        rows[:, cols] = part
        squares += jnp.sum(part * part, axis=1, keepdims=True)
    scale = lax.rsqrt(squares / stream.shape[1] + norm_eps)
    own[...] = rows[pl.ds((where[2] * 2 + where[3]) * 32, 32), :]
    for s in range(strips):
        cols = slice(s * STRIP, (s + 1) * STRIP)
        normed[:, cols] = (rows[:, cols] * scale * gain[:, cols]).astype(BF16)


def feedforward_kernel(n_gu, n_down, gu_places, down_places, where, x, *refs):
    gu_refs, down_refs = refs[:n_gu], refs[n_gu : n_gu + n_down]
    send, keep, gu, down, hidden, gu_sems, down_sems = refs[n_gu + n_down :]
    units = hidden.shape[1]

    def copies(places, sources, target, sems):
        out = []
        for k, (ref, row, dz, dy) in enumerate(places):
            to = lax.rem(where[0] + dz, 8) * 256 + lax.rem(where[1] + dy, 4) * 64
            out.append(
                pltpu.make_async_copy(
                    sources[ref].at[row : row + 64, :],
                    target.at[pl.ds(pl.multiple_of(to, 64), 64), :],
                    sems.at[k],
                )
            )
        return out

    gu_copies = copies(gu_places, gu_refs, gu, gu_sems)
    down_copies = copies(down_places, down_refs, down, down_sems)
    for c in gu_copies + down_copies:
        c.start()
    for c in gu_copies:
        c.wait()
    sums = jnp.dot(x[...], gu[...], preferred_element_type=F32)
    gate, up = sums[:, :units], sums[:, units:]
    hidden[...] = (gate / (1.0 + jnp.exp(-gate)) * up).astype(BF16)
    core = where[3]

    def rows_of(which):
        return jnp.concatenate(
            [hidden[pl.ds((2 * k + which) * 32, 32), :] for k in range(4)], axis=0
        )

    theirs, mine = rows_of(1 - core), rows_of(core)
    for c in down_copies:
        c.wait()
    for s in range(4):
        cols = slice(s * STRIP, (s + 1) * STRIP)
        send[:, cols] = lanes_contracted(theirs, down[cols, :]).astype(BF16)
        keep[:, cols] = lanes_contracted(mine, down[cols, :])


def around_z(own, far_left):
    left, right = [shift(own, "z", 1)], [shift(own, "z", -1)]
    for _ in range(2):
        left.append(shift(left[-1], "z", 1))
        right.append(shift(right[-1], "z", -1))
    far = shift(left[-1], "z", 1) if far_left else shift(right[-1], "z", -1)
    return left, right, far


def around(own, axis, far_left):
    left, right = shift(own, axis, 1), shift(own, axis, -1)
    far = shift(left, axis, 1) if far_left else shift(right, axis, -1)
    return [own, left, right, far]


def per_device(
    stream,
    first_group_queries,
    first_group_keys,
    first_group_values,
    first_gate_logits,
    first_decay_logits,
    second_group_queries,
    second_group_keys,
    second_group_values,
    second_gate_logits,
    second_decay_logits,
    position_log_decay,
    per_head_norm_gain,
    first_output_weight,
    second_output_weight,
    feedforward_norm_gain,
    gate_weight,
    up_weight,
    down_weight,
):
    tokens, width = stream.shape
    chips = SIZES["x"]
    part = tokens // (chips * 2)

    where = jnp.stack([lax.axis_index(a) for a in ("z", "y", "x", "c")]).astype(jnp.int32)
    gate_up = jnp.concatenate([gate_weight, up_weight], axis=1)
    left, right, far = around_z(gate_up, False)
    chunks = (
        ([gate_up], (0,), False),
        ([left[0], right[0], left[1], right[1]], (7, 1, 6, 2), True),
        ([left[2], right[2], far], (5, 3, 4), False),
    )
    gu_blocks, gu_places = [], []
    for blocks, offsets, far_left in chunks:
        both = jnp.concatenate(blocks, axis=0) if len(blocks) > 1 else blocks[0]
        for block, dy in zip(around(both, "y", far_left), (0, 3, 1, 2)):
            gu_places += [(len(gu_blocks), 64 * k, dz, dy) for k, dz in enumerate(offsets)]
            gu_blocks.append(block)

    down_four = jnp.concatenate(around(down_weight.T, "y", False), axis=0)
    left, right, far = around_z(down_four, True)
    down_blocks = [down_four, *left, *right, far]
    down_places = [
        (ref, 64 * k, dz, dy)
        for ref, dz in enumerate((0, 7, 6, 5, 1, 2, 3, 4))
        for k, dy in enumerate((0, 3, 1, 2))
    ]

    pos = position_log_decay.reshape(1, tokens)
    messages = call(
        states_kernel,
        jax.ShapeDtypeStruct((32, 24, DV), BF16),
        10**8,
        first_group_keys.T,
        first_group_values,
        first_decay_logits.T,
        second_group_keys,
        second_group_values,
        second_decay_logits,
        pos,
    )
    arrived = lax.all_to_all(messages, SP, 0, 0, tiled=True)

    out_own = jnp.concatenate([first_output_weight, second_output_weight], axis=0)
    out_same = around(out_own, "x", True)
    out_other = [shift(w, "c", 1) for w in out_same]

    local, query_ahead, query_behind = call(
        local_kernel,
        (
            jax.ShapeDtypeStruct((tokens, 2 * DV), F32),
            jax.ShapeDtypeStruct((tokens, 192), BF16),
            jax.ShapeDtypeStruct((tokens, 192), BF16),
        ),
        2 * 10**8,
        first_group_queries.T,
        first_group_keys.T,
        first_group_values,
        first_decay_logits.T,
        second_group_queries,
        second_group_keys,
        second_group_values,
        second_decay_logits,
        pos,
    )
    scanned = call(scan_kernel, jax.ShapeDtypeStruct((32, 16, DV), BF16), 10**7, arrived)
    states = lax.all_to_all(scanned, SP, 0, 0, tiled=True)
    mixed = call(
        finish_kernel,
        jax.ShapeDtypeStruct((tokens, 2 * DV), BF16),
        10**8,
        local,
        query_ahead,
        query_behind,
        states,
        first_gate_logits,
        second_gate_logits,
        per_head_norm_gain.reshape(1, DV),
    )
    left, right, far = shift(mixed, "x", 1), shift(mixed, "x", -1), shift(mixed, "x", 2)
    mixed_same = jnp.concatenate([mixed, left, right, far], axis=1)
    mixed_other = shift(mixed_same, "c", 1)
    normed, own = pl.pallas_call(
        residual_kernel,
        out_shape=(
            jax.ShapeDtypeStruct((tokens, width), BF16),
            jax.ShapeDtypeStruct((part, width), F32),
        ),
        in_specs=[SMEM, VMEM, VMEM, VMEM, VMEM] + [ANY] * 8,
        scratch_shapes=[
            pltpu.VMEM((width // STRIP, 2048, STRIP), BF16),
            pltpu.VMEM((tokens, width), F32),
            pltpu.SemaphoreType.DMA((width // STRIP, 8)),
        ],
        cost_estimate=pl.CostEstimate(flops=2 * 10**9, bytes_accessed=10**7, transcendentals=0),
    )(
        where,
        mixed_same,
        mixed_other,
        stream,
        feedforward_norm_gain.reshape(1, width),
        *out_same,
        *out_other,
    )
    units = gate_weight.shape[1]
    send, keep = pl.pallas_call(
        functools.partial(
            feedforward_kernel, len(gu_blocks), len(down_blocks), gu_places, down_places
        ),
        out_shape=(
            jax.ShapeDtypeStruct((tokens // 2, width), BF16),
            jax.ShapeDtypeStruct((tokens // 2, width), F32),
        ),
        in_specs=[SMEM, VMEM] + [ANY] * (len(gu_blocks) + len(down_blocks)),
        scratch_shapes=[
            pltpu.VMEM((width, 2 * units), BF16),
            pltpu.VMEM((width, units), BF16),
            pltpu.VMEM((tokens, units), BF16),
            pltpu.SemaphoreType.DMA((len(gu_places),)),
            pltpu.SemaphoreType.DMA((len(down_places),)),
        ],
        cost_estimate=pl.CostEstimate(flops=2 * 10**9, bytes_accessed=10**7, transcendentals=0),
    )(where, normed, *gu_blocks, *down_blocks)
    pair = (keep + shift(send, "c", 1).astype(F32)).astype(BF16)
    blocks = lax.all_to_all(pair.reshape(chips, part, width), "x", 0, 0, tiled=True)
    down_sum = jnp.sum(blocks.astype(F32), axis=0)
    return (own + 0.5 * down_sum).astype(BF16)


def solution(mesh):
    split = Mesh(mesh.devices.reshape(8, 4, 4, 2), ("z", "y", "x", "c"))
    placed = (
        P(SP, None),
        *(P(SP, TP),) * 10,
        P(SP),
        P(),
        P(TP, None),
        P(TP, None),
        P(),
        P(SP, TP),
        P(SP, TP),
        P(TP, SP),
    )
    return jax.shard_map(
        per_device, mesh=split, in_specs=placed, out_specs=P(SP + TP, None), check_vma=False
    )
```

```python
import jax
import jax.numpy as jnp
from jax import lax
from jax.experimental import pallas as pl
from jax.experimental.pallas import tpu as pltpu
from jax.sharding import Mesh
from jax.sharding import PartitionSpec as P

DV = 128
SP = ("z", "y")
TP = ("x", "c")
SIZES = {"z": 8, "y": 4, "x": 4, "c": 2}
HIGH = lax.Precision.HIGHEST
F32 = jnp.float32
BF16 = jnp.bfloat16


decay_softness = 16.0
norm_eps = 1e-06


def shift(value, axis, by):
    n = SIZES[axis]
    return lax.ppermute(value, axis, [(i, (i + by) % n) for i in range(n)])


def by_position(ref, n):
    value = ref[...].astype(F32)
    return value if value.shape[0] == n else value.T


def log_decays(decay_ref, n):
    d = by_position(decay_ref, n)
    return (jnp.minimum(d, 0.0) - jnp.log1p(jnp.exp(-jnp.abs(d)))) / decay_softness


def lower_mask(n):
    return lax.broadcasted_iota(jnp.int32, (n, n), 0) >= lax.broadcasted_iota(jnp.int32, (n, n), 1)


def position_sums(pos_ref):
    n = pos_ref.shape[1]
    rows = jnp.broadcast_to(pos_ref[...], (n, n))
    low = lower_mask(n)
    diag = lax.broadcasted_iota(jnp.int32, (n, n), 0) == lax.broadcasted_iota(jnp.int32, (n, n), 1)
    upto = jnp.sum(jnp.where(low, rows, 0.0), axis=1, keepdims=True)
    before = jnp.sum(jnp.where(low & ~diag, rows, 0.0), axis=1, keepdims=True)
    return upto, before


def running_sums(logd, upto, before):
    n = logd.shape[0]
    tri = jnp.where(lower_mask(n), 1.0, 0.0).astype(F32)
    cum = jnp.dot(tri, logd, precision=HIGH, preferred_element_type=F32)
    return cum + upto, (cum - logd) + before


def rows_contracted(a, b, precision=None):
    return lax.dot_general(
        a, b, (((0,), (0,)), ((), ())), precision=precision, preferred_element_type=F32
    )


def lanes_contracted(a, b):
    return lax.dot_general(a, b, (((1,), (1,)), ((), ())), preferred_element_type=F32)


def states_kernel(ka, va, da, kb, vb, db, pos, msg):
    upto, before = position_sums(pos)
    n = pos.shape[1]
    pos_total = jnp.sum(pos[...], axis=1, keepdims=True)
    ones = jnp.ones((n, DV), F32)
    at = 0
    for k_ref, v_ref, d_ref in ((kb, vb, db), (ka, va, da)):
        logd = log_decays(d_ref, n)
        upto_l, before_l = running_sums(logd, upto, before)
        total = upto_l[n - 1 : n, :]
        key = by_position(k_ref, n)
        value = v_ref[...]
        ahead = rows_contracted((key * jnp.exp(total - upto_l)).astype(BF16), value)
        behind = rows_contracted((key * jnp.exp(before_l)).astype(BF16), value)
        totals = rows_contracted(logd, ones, HIGH) + pos_total
        high = totals.astype(BF16).astype(F32)
        lane = lax.broadcasted_iota(jnp.int32, totals.shape, 1)
        both = jnp.where(lane < 64, high, totals - high)
        groups = logd.shape[1] // 8
        part = jnp.concatenate(
            [x.reshape(groups, 8, DV) for x in (ahead, behind, both)], axis=1
        )
        msg[at : at + groups] = part.astype(BF16)
        at += groups
    msg[at:] = jnp.zeros((msg.shape[0] - at, *msg.shape[1:]), BF16)


def scan_kernel(msg, out):
    n = msg.shape[0]
    blocks = msg[...].astype(F32)
    decay = jnp.exp(blocks[:, 16:24, 0:1] + blocks[:, 16:24, 64:65])
    run = jnp.zeros((8, DV), F32)
    ahead = []
    for k in range(n):
        ahead.append(run)
        run = run * decay[k] + blocks[k, 0:8, :]
    run = jnp.zeros((8, DV), F32)
    behind = []
    for k in reversed(range(n)):
        behind.append(run)
        run = run * decay[k] + blocks[k, 8:16, :]
    behind.reverse()
    for k in range(n):
        out[k] = jnp.concatenate([ahead[k], behind[k]], axis=0).astype(BF16)


def local_kernel(qa, ka, va, da, qb, kb, vb, db, pos, out, qf_out, qb_out):
    n = pos.shape[1]
    half = n // 2
    upto, before = position_sums(pos)
    low = lower_mask(half)
    up = lax.broadcasted_iota(jnp.int32, (half, half), 0) <= lax.broadcasted_iota(
        jnp.int32, (half, half), 1
    )
    for g, (q_ref, k_ref, v_ref, d_ref) in enumerate(((qa, ka, va, da), (qb, kb, vb, db))):
        inc, exc = running_sums(log_decays(d_ref, n), upto, before)
        q = by_position(q_ref, n)
        k = by_position(k_ref, n)
        total = inc[n - 1 : n, :]
        lo = 0 if g == 1 else 128
        width = q.shape[1]
        qf_out[:, lo : lo + width] = (q * jnp.exp(inc)).astype(BF16)
        qb_out[:, lo : lo + width] = (q * jnp.exp(total - exc)).astype(BF16)
        diag = []
        for b in range(2):
            s = slice(b * half, (b + 1) * half)
            m = inc[b * half + half // 2 - 1 : b * half + half // 2, :]
            ahead = lanes_contracted(
                (q[s] * jnp.exp(inc[s] - m)).astype(BF16), (k[s] * jnp.exp(m - inc[s])).astype(BF16)
            )
            behind = lanes_contracted(
                (q[s] * jnp.exp(m - exc[s])).astype(BF16), (k[s] * jnp.exp(exc[s] - m)).astype(BF16)
            )
            diag.append(jnp.where(low, ahead, 0.0) + jnp.where(up, behind, 0.0))
        m = inc[half - 1 : half, :]
        first, second = slice(0, half), slice(half, n)
        down = lanes_contracted(
            (q[second] * jnp.exp(inc[second] - m)).astype(BF16),
            (k[first] * jnp.exp(m - inc[first])).astype(BF16),
        )
        upper = lanes_contracted(
            (q[first] * jnp.exp(m - exc[first])).astype(BF16),
            (k[second] * jnp.exp(exc[second] - m)).astype(BF16),
        )
        weights = jnp.concatenate(
            [
                jnp.concatenate([diag[0], upper], axis=1),
                jnp.concatenate([down, diag[1]], axis=1),
            ],
            axis=0,
        ).astype(BF16)
        out[:, g * DV : (g + 1) * DV] = jnp.dot(weights, v_ref[...], preferred_element_type=F32)


def finish_kernel(local, qf, qb, states, ga, gb, gain, out):
    groups = states[...].astype(F32)[:24]
    ahead = groups[:, 0:8, :].reshape(192, DV).astype(BF16)
    behind = groups[:, 8:16, :].reshape(192, DV).astype(BF16)
    for g, gate_ref in enumerate((ga, gb)):
        lo, hi = (0, 128) if g == 1 else (128, 192)
        both = (
            local[:, g * DV : (g + 1) * DV]
            + jnp.dot(qf[:, lo:hi], ahead[lo:hi], preferred_element_type=F32)
            + jnp.dot(qb[:, lo:hi], behind[lo:hi], preferred_element_type=F32)
        )
        scale = lax.rsqrt(jnp.mean(both * both, axis=-1, keepdims=True) + norm_eps)
        gate = gate_ref[...].astype(F32)
        silu = gate / (1.0 + jnp.exp(-gate))
        out[:, g * DV : (g + 1) * DV] = (both * scale * gain[...] * silu).astype(BF16)


def vmem(mib):
    return pltpu.CompilerParams(vmem_limit_bytes=mib * 2**20)


def call(kernel, out_shape, flops, *args):
    return pl.pallas_call(
        kernel,
        out_shape=out_shape,
        compiler_params=vmem(8),
        cost_estimate=pl.CostEstimate(flops=flops, bytes_accessed=10**6, transcendentals=10**5),
    )(*args)


ANY = pl.BlockSpec(memory_space=pl.ANY)
VMEM = pl.BlockSpec(memory_space=pltpu.VMEM)
SMEM = pl.BlockSpec(memory_space=pltpu.SMEM)
STRIP = 512


def residual_kernel(where, same, other, stream, gain, *refs):
    weights, (normed, own, scratch, rows, sems) = refs[:8], refs[8:]
    strips = stream.shape[1] // STRIP

    def copy(k, s):
        cols = slice(s * STRIP, (s + 1) * STRIP)
        return pltpu.make_async_copy(
            weights[k].at[:, cols], scratch.at[s, k * 256 : (k + 1) * 256, :], sems.at[s, k]
        )

    for s in range(strips):
        for k in range(8):
            copy(k, s).start()
    squares = jnp.zeros((stream.shape[0], 1), F32)
    for s in range(strips):
        for k in range(8):
            copy(k, s).wait()
        cols = slice(s * STRIP, (s + 1) * STRIP)
        part = (
            stream[:, cols].astype(F32)
            + jnp.dot(same[...], scratch[s, :1024, :], preferred_element_type=F32)
            + jnp.dot(other[...], scratch[s, 1024:, :], preferred_element_type=F32)
        )
        rows[:, cols] = part
        squares += jnp.sum(part * part, axis=1, keepdims=True)
    scale = lax.rsqrt(squares / stream.shape[1] + norm_eps)
    own[...] = rows[pl.ds((where[2] * 2 + where[3]) * 32, 32), :]
    for s in range(strips):
        cols = slice(s * STRIP, (s + 1) * STRIP)
        normed[:, cols] = (rows[:, cols] * scale * gain[:, cols]).astype(BF16)


DY = (0, 3, 1, 2)
DZ_NEAR = (0, 7, 1, 6)
DZ_FAR = (2, 5, 3, 4)


def feedforward_kernel(where, x, *refs):
    blocks, (send, keep, weights, hidden, sems) = refs[:12], refs[12:]
    units = hidden.shape[1]
    core = where[3]

    def copy(ref, slot, k, dz, dy):
        to = lax.rem(where[0] + dz, 8) * 256 + lax.rem(where[1] + dy, 4) * 64
        return pltpu.make_async_copy(
            ref.at[64 * k : 64 * k + 64, :],
            weights.at[pl.ds(pl.multiple_of(to, 64), 64), :],
            sems.at[slot, k],
        )

    steps = ((0, 0), (7, 3), (1, 1), (6, 2))
    shared = [
        copy(
            blocks[slot],
            slot,
            k,
            jnp.where(core == 0, dz, DZ_NEAR[k]),
            jnp.where(core == 0, DY[k], dy),
        )
        for slot, (dz, dy) in enumerate(steps)
        for k in range(4)
    ]
    for c in shared:
        c.start()

    def rest(which):
        if which == 0:
            return [
                copy(blocks[4 + i], 4 + i, k, dz, DY[k])
                for i, dz in enumerate((2, 5, 3, 4))
                for k in range(4)
            ]
        return [
            copy(blocks[8 + i], 4 + i, k, DZ_FAR[k], dy)
            for i, dy in enumerate((0, 3, 1, 2))
            for k in range(4)
        ]

    for which in range(2):

        @pl.when(core == which)
        def _():
            for c in rest(which):
                c.start()

    for c in shared + rest(0):
        c.wait()
    sums = jnp.dot(x[...], weights[:, : 2 * units], preferred_element_type=F32)
    gate, up = sums[:, :units], sums[:, units:]
    hidden[...] = (gate / (1.0 + jnp.exp(-gate)) * up).astype(BF16)

    def rows_of(which):
        return jnp.concatenate(
            [hidden[pl.ds((2 * k + which) * 32, 32), :] for k in range(4)], axis=0
        )

    theirs, mine = rows_of(1 - core), rows_of(core)
    for s in range(4):
        cols = slice(s * STRIP, (s + 1) * STRIP)
        down = weights[cols, 2 * units : 3 * units]
        send[:, cols] = lanes_contracted(theirs, down).astype(BF16)
        keep[:, cols] = lanes_contracted(mine, down)


def join_kernel(*refs):
    at = 0
    for ref in refs[:-1]:
        refs[-1][at : at + ref.shape[0], :] = ref[...]
        at += ref.shape[0]


def joined(*blocks):
    rows = sum(b.shape[0] for b in blocks)
    return pl.pallas_call(
        join_kernel,
        out_shape=jax.ShapeDtypeStruct((rows, blocks[0].shape[1]), blocks[0].dtype),
        in_specs=[VMEM] * len(blocks),
        out_specs=VMEM,
        compiler_params=vmem(6),
        cost_estimate=pl.CostEstimate(flops=10**7, bytes_accessed=10**6, transcendentals=0),
    )(*blocks)


def routed(value, *moves):
    pairs = []
    for i in range(256):
        at = {"z": i // 32, "y": i // 8 % 4, "x": i // 2 % 4, "c": i % 2}
        if moves[at["c"]] is not None:
            axis, by = moves[at["c"]]
            at[axis] = (at[axis] + by) % SIZES[axis]
            pairs.append((i, ((at["z"] * 4 + at["y"]) * 4 + at["x"]) * 2 + at["c"]))
    return lax.ppermute(value, SP + TP, pairs)


def gathered_weights(own):
    near_1 = routed(own, ("y", 1), ("z", 1))
    near_2 = routed(own, ("y", -1), ("z", -1))
    near_3 = routed(near_1, ("y", 1), ("z", 1))
    four = joined(own, near_1, near_2, near_3)
    left = routed(four, ("z", 1), ("y", 1))
    right = routed(four, ("z", -1), ("y", -1))
    left_2 = routed(left, ("z", 1), ("y", 1))
    far_1 = routed(near_2, None, ("z", -1))
    far_2 = routed(near_3, None, ("z", 1))
    far_3 = routed(far_1, None, ("z", -1))
    far_4 = routed(far_2, None, ("z", 1))
    far = joined(far_1, far_2, far_3, far_4)
    right_2 = routed(right, ("z", -1), None)
    far_left = routed(far, None, ("y", 1))
    far_right = routed(far, None, ("y", -1))
    left_3 = routed(left_2, ("z", 1), None)
    right_3 = routed(right_2, ("z", -1), None)
    far_right_2 = routed(far_right, None, ("y", -1))
    right_4 = routed(right_3, ("z", -1), None)
    return (
        [four, left, right, left_2]
        + [right_2, left_3, right_3, right_4]
        + [far, far_left, far_right, far_right_2]
    )


def around(own, axis, far_left):
    left, right = shift(own, axis, 1), shift(own, axis, -1)
    far = shift(left, axis, 1) if far_left else shift(right, axis, -1)
    return [own, left, right, far]


def per_device(
    stream,
    first_group_queries,
    first_group_keys,
    first_group_values,
    first_gate_logits,
    first_decay_logits,
    second_group_queries,
    second_group_keys,
    second_group_values,
    second_gate_logits,
    second_decay_logits,
    position_log_decay,
    per_head_norm_gain,
    first_output_weight,
    second_output_weight,
    feedforward_norm_gain,
    gate_weight,
    up_weight,
    down_weight,
):
    tokens, width = stream.shape
    chips = SIZES["x"]
    part = tokens // (chips * 2)

    where = jnp.stack([lax.axis_index(a) for a in ("z", "y", "x", "c")]).astype(jnp.int32)
    weights = gathered_weights(
        jnp.concatenate(
            [gate_weight, up_weight, down_weight.T, jnp.zeros((64, 64), BF16)], axis=1
        )
    )

    pos = position_log_decay.reshape(1, tokens)
    messages = call(
        states_kernel,
        jax.ShapeDtypeStruct((32, 24, DV), BF16),
        10**8,
        first_group_keys.T,
        first_group_values,
        first_decay_logits.T,
        second_group_keys,
        second_group_values,
        second_decay_logits,
        pos,
    )
    arrived = lax.all_to_all(messages, SP, 0, 0, tiled=True)

    out_own = joined(first_output_weight, second_output_weight)
    out_same = around(out_own, "x", True)
    out_other = [shift(w, "c", 1) for w in out_same]

    local, query_ahead, query_behind = call(
        local_kernel,
        (
            jax.ShapeDtypeStruct((tokens, 2 * DV), F32),
            jax.ShapeDtypeStruct((tokens, 192), BF16),
            jax.ShapeDtypeStruct((tokens, 192), BF16),
        ),
        2 * 10**8,
        first_group_queries.T,
        first_group_keys.T,
        first_group_values,
        first_decay_logits.T,
        second_group_queries,
        second_group_keys,
        second_group_values,
        second_decay_logits,
        pos,
    )
    scanned = call(scan_kernel, jax.ShapeDtypeStruct((32, 16, DV), BF16), 10**7, arrived)
    states = lax.all_to_all(scanned, SP, 0, 0, tiled=True)
    mixed = call(
        finish_kernel,
        jax.ShapeDtypeStruct((tokens, 2 * DV), BF16),
        10**8,
        local,
        query_ahead,
        query_behind,
        states,
        first_gate_logits,
        second_gate_logits,
        per_head_norm_gain.reshape(1, DV),
    )
    left, right, far = shift(mixed, "x", 1), shift(mixed, "x", -1), shift(mixed, "x", 2)
    mixed_same = jnp.concatenate([mixed, left, right, far], axis=1)
    mixed_other = shift(mixed_same, "c", 1)
    normed, own = pl.pallas_call(
        residual_kernel,
        out_shape=(
            jax.ShapeDtypeStruct((tokens, width), BF16),
            jax.ShapeDtypeStruct((part, width), F32),
        ),
        in_specs=[SMEM, VMEM, VMEM, VMEM, VMEM] + [ANY] * 8,
        scratch_shapes=[
            pltpu.VMEM((width // STRIP, 2048, STRIP), BF16),
            pltpu.VMEM((tokens, width), F32),
            pltpu.SemaphoreType.DMA((width // STRIP, 8)),
        ],
        compiler_params=vmem(20),
        cost_estimate=pl.CostEstimate(flops=2 * 10**9, bytes_accessed=10**7, transcendentals=0),
    )(
        where,
        mixed_same,
        mixed_other,
        stream,
        feedforward_norm_gain.reshape(1, width),
        *out_same,
        *out_other,
    )
    units = gate_weight.shape[1]
    send, keep = pl.pallas_call(
        feedforward_kernel,
        out_shape=(
            jax.ShapeDtypeStruct((tokens // 2, width), BF16),
            jax.ShapeDtypeStruct((tokens // 2, width), F32),
        ),
        in_specs=[SMEM, VMEM] + [ANY] * 12,
        scratch_shapes=[
            pltpu.VMEM((width, 3 * units + 64), BF16),
            pltpu.VMEM((tokens, units), BF16),
            pltpu.SemaphoreType.DMA((8, 4)),
        ],
        compiler_params=vmem(20),
        cost_estimate=pl.CostEstimate(flops=2 * 10**9, bytes_accessed=10**7, transcendentals=0),
    )(where, normed, *weights)
    pair = (keep + shift(send, "c", 1).astype(F32)).astype(BF16)
    blocks = lax.all_to_all(pair.reshape(chips, part, width), "x", 0, 0, tiled=True)
    down_sum = jnp.sum(blocks.astype(F32), axis=0)
    return (own + 0.5 * down_sum).astype(BF16)


def solution(mesh):
    split = Mesh(mesh.devices.reshape(8, 4, 4, 2), ("z", "y", "x", "c"))
    placed = (
        P(SP, None),
        *(P(SP, TP),) * 10,
        P(SP),
        P(),
        P(TP, None),
        P(TP, None),
        P(),
        P(SP, TP),
        P(SP, TP),
        P(TP, SP),
    )
    return jax.shard_map(
        per_device, mesh=split, in_specs=placed, out_specs=P(SP + TP, None), check_vma=False
    )
```
